32 devices in a mesh: ep: 8 (over z, core), tp: 4 (over y, x).
Axes of the slice: x: 2, y: 2, z: 4, core: 2. Of those that a mesh axis runs over, the one named last changes fastest.
Arguments:
- query_input: bfloat16 [4096, 2048], P('ep', 'tp'), may hold values from -6 to 6
- key_input: bfloat16 [4096, 1024], P('ep', 'tp'), may hold values from -6 to 6
- value_input: bfloat16 [4096, 1024], P('ep', 'tp'), may hold values from -64 to 64
- query_gain: float32 [64], replicated, may hold values from 0.5 to 6
- key_gain: float32 [64], replicated, may hold values from 0.5 to 6
- mixer_out: bfloat16 [2048, 4096], P(None, 'tp'), may hold values from -0.125 to 0.125
- moe_input: bfloat16 [2048, 4096], P('ep'), may hold values from -6 to 6
- moe_gain: float32 [4096], replicated, may hold values from 0.1 to 1.9
- routes: int32 [2048, 2], P('ep'), may hold values from 0 to 7, all different within a row; in each aligned block of 256 rows (0 to 255, 256 to 511, ...) at most 96 rows name the same one
- route_weight: float32 [2048, 2], P('ep'), may hold values from 0.1 to 1
- expert_gate: bfloat16 [8, 4096, 1024], P('ep', None, 'tp'), may hold values from -0.09375 to 0.09375
- expert_up: bfloat16 [8, 4096, 1024], P('ep', None, 'tp'), may hold values from -0.09375 to 0.09375
- expert_down: bfloat16 [8, 1024, 4096], P('ep', None, 'tp'), may hold values from -0.1875 to 0.1875
Outputs:
- attn_mixed: bfloat16 [4096, 4096], P('ep', 'tp')
- moe_out: bfloat16 [2048, 4096], P('ep', 'tp')
The draws below stay inside these ranges and needn't reach their ends.
Inputs may be any that keep to these rules, and one draw needn't show every extreme that they name: `routes`: each row names 2 different experts. In the rows of one index of ep (aligned blocks of 256 rows) no expert is named by more than 96 rows, and in every draw some block has an expert named by exactly 96 rows.
All inputs are finite; a program needn't handle non-finite values.
Results may differ from the reference program's by a relative error of at most 0.0095.
The reference program's roundings to bfloat16 on the way count: a program that leaves them out, or rounds other values in their place, can miss the bound.
Values may be sent and summed in bfloat16 or wider, within the bound.
A program may use at most 64 MiB of HBM per device.

```python
import math
import jax
import jax.numpy as jnp
import numpy as np
from jax import lax

D = 4096
HEADS = 32
KV_HEADS = 16
HEAD_DIM = 64
FF = 1024
GRID_W = 64
TOP_K = 2
MOE_TOK = 256
SEQ_LEN = 4096
MOE_TOKENS = 2048
EXPERTS = 8
CAP = 96
N_EP = 8


def draw_query_input(key, part):
    column_count = HEADS * HEAD_DIM
    samples = jnp.clip(jax.random.normal(jax.random.fold_in(key, 101), (SEQ_LEN, column_count), jnp.float32), -6.0, 6.0)
    return samples.astype(jnp.bfloat16)


def draw_key_input(key, part):
    column_count = KV_HEADS * HEAD_DIM
    samples = jnp.clip(jax.random.normal(jax.random.fold_in(key, 202), (SEQ_LEN, column_count), jnp.float32), -6.0, 6.0)
    return samples.astype(jnp.bfloat16)


def draw_query_gain(key, part):
    spread = jax.random.uniform(jax.random.fold_in(key, 303), (HEAD_DIM,), jnp.float32, jnp.log(0.5), jnp.log(2.0))
    gains = jnp.exp(spread)
    return gains.astype(jnp.float32)


def draw_key_gain(key, part):
    spread = jax.random.uniform(jax.random.fold_in(key, 404), (HEAD_DIM,), jnp.float32, jnp.log(0.5), jnp.log(2.0))
    gains = jnp.exp(spread)
    return gains.astype(jnp.float32)


def block_levels(key, shape, pieces, least, high):
    def one(axis_at, blocks):
        heights = jax.random.uniform(jax.random.fold_in(jax.random.fold_in(key, 6), axis_at), (blocks,), jnp.float32, least / len(pieces), high / len(pieces))
        return jnp.repeat(jnp.exp(heights), shape[axis_at] // blocks).reshape((-1,) + (1,) * (len(shape) - axis_at - 1))

    factor_of = one(*pieces[0])
    for cut in pieces[1:]:
        factor_of = factor_of * one(*cut)
    return factor_of


def routed_block(stream_key, own, number, rows, amount, top, bound, skew):
    order = jax.random.permutation(stream_key, amount)
    packed, common = portions_of(amount, rows * top, bound, skew, True), portions_of(amount, rows * top, bound, skew, False)
    places = jnp.arange(amount)

    def named(tallies, rotation):
        used = int((tallies > 0).sum())
        fixed = max(1, used // 4)
        moved = fixed + (places - fixed + rotation * (used - fixed)) % max(1, amount - fixed)
        return jnp.zeros((amount,), jnp.int32).at[order[jnp.where(places < fixed, places, moved)]].set(jnp.asarray(tallies, jnp.int32))

    tallies = jnp.where(number % 4 == 0, named(packed, number // 4), named(common, number - number // 4 - 1))
    mixed = jax.random.permutation(jax.random.fold_in(own, 3), amount)
    source_of, sink = mixed[0:amount // 2 * 2:2], mixed[1:amount // 2 * 2:2]
    slack = jnp.minimum(tallies[source_of] - 1, bound - tallies[sink]) // 2
    slack = jnp.where((source_of == order[0]) | (sink == order[0]) | (tallies[sink] == 0), 0, jnp.maximum(slack, 0))
    moved = jax.random.randint(jax.random.fold_in(own, 4), (amount // 2,), 0, 1 << 20) % (slack + 1)
    tallies = tallies.at[source_of].add(-moved).at[sink].add(moved)
    labels = jnp.searchsorted(jnp.cumsum(tallies), jnp.arange(rows * top), side="right").astype(jnp.int32)
    listing = labels.reshape(top, rows).T
    listing = listing[jax.random.permutation(jax.random.fold_in(own, 1), rows)]
    rotation = jax.random.randint(jax.random.fold_in(own, 2), (rows, 1), 0, top)
    return jnp.take_along_axis(listing, (jnp.arange(top)[None, :] + rotation) % top, axis=1)


def portions_of(amount, total, reach, skew, full):
    weights = [(1 << 20) // math.isqrt(rank ** skew) + 1 for rank in range(1, amount + 1)]
    largest = reach if full else min(reach, max(-(-total // amount), total * weights[0] // sum(weights)))
    least = 1 if total - largest >= amount - 1 else 0
    counts, rest = [largest] + [least] * (amount - 1), total - largest - least * (amount - 1)
    while rest > 0:
        movable = [i for i in range(1, amount) if counts[i] < largest] or [i for i in range(1, amount) if counts[i] < reach]
        pool, left = sum([weights[i] for i in movable]), rest
        for i in movable:
            addition = min(reach - counts[i], max(1, left * weights[i] // pool), rest)
            counts[i] = counts[i] + addition
            rest = rest - addition
    return np.array(counts)


def scatter_about(stream_key, dims, scale, bound, cuts=(), held_as=jnp.bfloat16):
    result = jax.random.normal(stream_key, dims, jnp.float32) * scale
    if len(cuts) > 0:
        result = block_levels(stream_key, dims, cuts, -0.22, 0.18) * result
    return jnp.clip(result, min=-bound, max=bound).astype(held_as)


def setup_inputs(seed: int = 0) -> dict:
    streams_of = jax.random.split(jax.random.key(seed), 14)
    query_input = draw_query_input(jax.random.fold_in(streams_of[13], 71), 0)
    key_input = draw_key_input(jax.random.fold_in(streams_of[13], 71), 0)
    value_input = jnp.clip(jax.random.uniform(streams_of[2], (SEQ_LEN, KV_HEADS * HEAD_DIM), jnp.float32, -64.0, 64.0) * block_levels(streams_of[2], (SEQ_LEN, KV_HEADS * HEAD_DIM), ((0, 8), (1, 4)), -0.4, 0.0), -64.0, 64.0).astype(jnp.bfloat16)
    query_gain = draw_query_gain(jax.random.fold_in(streams_of[13], 71), 0)
    key_gain = draw_key_gain(jax.random.fold_in(streams_of[13], 71), 0)
    mixer_out = scatter_about(streams_of[5], (HEADS * HEAD_DIM, D), (HEADS * HEAD_DIM) ** -0.5, 0.125, ((1, 4),))
    moe_input = scatter_about(streams_of[6], (MOE_TOKENS, D), 1.0, 6.0, ((0, 8),))
    moe_gain = jnp.clip(1.0 + 0.18 * jax.random.normal(streams_of[7], (D,), jnp.float32), 0.1, 1.9)
    routes_keys = jax.random.split(jax.random.fold_in(streams_of[8], 1), MOE_TOKENS // MOE_TOK)
    routes_turns = jax.random.permutation(jax.random.fold_in(streams_of[8], 3), MOE_TOKENS // MOE_TOK)
    routes = jax.vmap(lambda own, number: routed_block(jax.random.fold_in(streams_of[8], 2), own, number, MOE_TOK, EXPERTS, TOP_K, CAP, 1))(routes_keys, routes_turns).reshape((MOE_TOKENS, TOP_K))
    route_weight = jnp.clip(jnp.exp(math.log(1.0) - 2.3025851 * jax.random.uniform(streams_of[9], (MOE_TOKENS, TOP_K), jnp.float32) ** block_levels(streams_of[9], (MOE_TOKENS, TOP_K), ((0, 8),), -0.2, 0.2)), 0.1, 1.0)
    expert_gate = scatter_about(streams_of[10], (EXPERTS, D, FF), D ** -0.5, 0.09375, ((0, 8), (2, 4)))
    expert_up = scatter_about(streams_of[11], (EXPERTS, D, FF), D ** -0.5, 0.09375, ((0, 8), (2, 4)))
    expert_down = scatter_about(streams_of[12], (EXPERTS, FF, D), FF ** -0.5, 0.1875, ((0, 8), (2, 4)))
    return {"query_input": query_input, "key_input": key_input, "value_input": value_input, "query_gain": query_gain, "key_gain": key_gain, "mixer_out": mixer_out, "moe_input": moe_input, "moe_gain": moe_gain, "routes": routes, "route_weight": route_weight, "expert_gate": expert_gate, "expert_up": expert_up, "expert_down": expert_down}


epsilon = 1e-06
base_theta = 10000.0

def rope_tables(positions, head_width):
    quarter = head_width // 4
    inverse = base_theta ** (-jnp.arange(quarter, dtype=jnp.float32) / quarter)
    grid_row = (positions // GRID_W).astype(jnp.float32)
    grid_col = (positions % GRID_W).astype(jnp.float32)
    angles = jnp.concatenate([grid_row[:, None] * inverse[None, :], grid_col[:, None] * inverse[None, :]], axis=1)
    return (jnp.cos(angles), jnp.sin(angles))

def head_norm(heads_in, gain):
    return heads_in * lax.rsqrt(lax.optimization_barrier(jnp.mean(heads_in * heads_in, axis=-1, keepdims=True)) + epsilon) * gain

def rotate(heads_in, cosine, sine_table):
    half_width = heads_in.shape[-1] // 2
    first_half = heads_in[..., :half_width]
    second_half = heads_in[..., half_width:]
    cos_rows = cosine[:, None, :]
    sin_rows = sine_table[:, None, :]
    return jnp.concatenate([first_half * cos_rows - second_half * sin_rows, first_half * sin_rows + second_half * cos_rows], axis=-1)

def slot_places(route_block, expert_count, capacity):
    flat_routes = route_block.reshape(-1)
    one_hot = (flat_routes[:, None] == jnp.arange(expert_count, dtype=jnp.int32)[None, :]).astype(jnp.int32)
    earlier = jnp.cumsum(one_hot, axis=0) - one_hot
    return (flat_routes * capacity + lax.optimization_barrier(jnp.sum(earlier * one_hot, axis=1))).astype(jnp.int32)

def fill_sources(places, token_count, top_count, slot_total):
    source_rows = jnp.full((slot_total,), token_count, jnp.int32)
    pair_rows = (jnp.arange(token_count * top_count, dtype=jnp.int32) // top_count).astype(jnp.int32)
    return source_rows.at[places].set(pair_rows)

def attend(query_rot, key_rot, value_input):
    seq_len = query_rot.shape[0]
    group_size = HEADS // KV_HEADS
    block_len = math.gcd(seq_len, 128)
    key_all = key_rot.astype(jnp.float32)
    value_all = value_input.astype(jnp.float32).reshape(seq_len, KV_HEADS, HEAD_DIM)
    blocks = query_rot.astype(jnp.float32).reshape(seq_len // block_len, block_len, KV_HEADS, group_size, HEAD_DIM)
    score_scale = HEAD_DIM ** (-0.5)

    def one_block(query_block):
        scores = jnp.einsum('qkgd,skd->kgqs', query_block, key_all) * score_scale
        largest = lax.optimization_barrier(jnp.max(scores, axis=-1, keepdims=True))
        weights = jnp.exp(scores - largest)
        denominator = lax.optimization_barrier(jnp.sum(weights, axis=-1))
        rounded = lax.optimization_barrier(weights.astype(jnp.bfloat16)).astype(jnp.float32)
        numerator = jnp.einsum('kgqs,skd->qkgd', rounded, value_all)
        return numerator / jnp.transpose(denominator, (2, 0, 1))[..., None]
    attended = lax.map(one_block, blocks)
    return attended.reshape(seq_len, HEADS * HEAD_DIM).astype(jnp.bfloat16)

def experts_layer(moe_input, moe_gain, routes, route_weight, expert_gate, expert_up, expert_down):
    features = moe_input.astype(jnp.float32)
    normed = (features * lax.rsqrt(lax.optimization_barrier(jnp.mean(features * features, axis=-1, keepdims=True)) + epsilon) * moe_gain).astype(jnp.bfloat16)
    blocks = normed.reshape(N_EP, MOE_TOK, D)
    places = jax.vmap(lambda route_block: slot_places(route_block, EXPERTS, CAP))(routes.reshape(N_EP, MOE_TOK, TOP_K))
    sources = jax.vmap(lambda place_row: fill_sources(place_row, MOE_TOK, TOP_K, EXPERTS * CAP))(places)
    padded = jnp.concatenate([blocks, jnp.zeros((N_EP, 1, D), jnp.bfloat16)], axis=1)
    gathered = jax.vmap(lambda padded_block, source_row: padded_block[source_row])(padded, sources)
    per_expert = gathered.reshape(N_EP, EXPERTS, CAP, D).transpose(1, 0, 2, 3).reshape(EXPERTS, N_EP * CAP, D)

    def one_expert(operands):
        expert_rows, gate_matrix, up_matrix, down_matrix = operands
        gate_hidden = jnp.dot(expert_rows, gate_matrix, preferred_element_type=jnp.float32)
        up_hidden = jnp.dot(expert_rows, up_matrix, preferred_element_type=jnp.float32)
        hidden = (jax.nn.silu(gate_hidden) * up_hidden).astype(jnp.bfloat16)
        return jnp.dot(hidden, down_matrix, preferred_element_type=jnp.float32).astype(jnp.bfloat16)
    outputs = lax.map(one_expert, (per_expert, expert_gate, expert_up, expert_down))
    returned = outputs.reshape(EXPERTS, N_EP, CAP, D).transpose(1, 0, 2, 3).reshape(N_EP, EXPERTS * CAP, D)
    picked = jax.vmap(lambda returned_block, place_row: returned_block[place_row])(returned, places)
    picked = picked.reshape(N_EP * MOE_TOK, TOP_K, D).astype(jnp.float32)
    shares = route_weight / lax.optimization_barrier(jnp.sum(route_weight, axis=-1, keepdims=True))
    return lax.optimization_barrier(jnp.sum(picked * shares[:, :, None], axis=1)).astype(jnp.bfloat16)

def reference(query_input, key_input, value_input, query_gain, key_gain, mixer_out, moe_input, moe_gain, routes, route_weight, expert_gate, expert_up, expert_down):
    seq_len = query_input.shape[0]
    positions = jnp.arange(seq_len, dtype=jnp.int32)
    cosine, sine_table = rope_tables(positions, HEAD_DIM)
    query_heads = query_input.astype(jnp.float32).reshape(seq_len, HEADS, HEAD_DIM)
    key_heads = key_input.astype(jnp.float32).reshape(seq_len, KV_HEADS, HEAD_DIM)
    query_rot = rotate(head_norm(query_heads, query_gain), cosine, sine_table).astype(jnp.bfloat16)
    key_rot = rotate(head_norm(key_heads, key_gain), cosine, sine_table).astype(jnp.bfloat16)
    attended = attend(query_rot, key_rot, value_input)
    attn_mixed = jnp.dot(attended, mixer_out, preferred_element_type=jnp.float32).astype(jnp.bfloat16)
    moe_out = experts_layer(moe_input, moe_gain, routes, route_weight, expert_gate, expert_up, expert_down)
    return (attn_mixed, moe_out)
```

```python
import functools
import math

import jax
import jax.numpy as jnp
from jax import lax
from jax.experimental import pallas as pl
from jax.experimental.pallas import tpu as pltpu
from jax.sharding import PartitionSpec as P

GRID_W = 64
CORES = 2

epsilon = 1e-06
base_theta = 10000.0


def rope_tables(positions, head_width):
    quarter = head_width // 4
    inverse = base_theta ** (-jnp.arange(quarter, dtype=jnp.float32) / quarter)
    grid_row = (positions // GRID_W).astype(jnp.float32)
    grid_col = (positions % GRID_W).astype(jnp.float32)
    angles = jnp.concatenate(
        [grid_row[:, None] * inverse[None, :], grid_col[:, None] * inverse[None, :]], axis=1
    )
    return (jnp.cos(angles), jnp.sin(angles))


def norm_rotate(columns, gain, cosine, sine, head_width):
    width = columns.shape[1]
    heads = width // head_width
    lane = jnp.arange(width)
    same_head = (lane[:, None] // head_width == lane[None, :] // head_width).astype(jnp.float32)
    half = head_width // 2
    within = lane % head_width
    partner = jnp.where(within < half, lane + half, lane - half)
    swap = (lane[:, None] == partner[None, :]).astype(jnp.bfloat16)
    values = columns.astype(jnp.float32)
    mean = (
        jnp.dot(values * values, same_head, precision=lax.Precision.HIGHEST) / head_width
    )
    scale = lax.rsqrt(mean + epsilon)
    swapped = jnp.dot(columns, swap, preferred_element_type=jnp.float32)
    gain_here = jnp.tile(gain, heads)[None, :]
    gain_swapped = jnp.tile(jnp.roll(gain, half), heads)[None, :]
    cos_here = jnp.tile(cosine, (1, 2 * heads))
    sin_here = jnp.tile(jnp.concatenate([-sine, sine], axis=1), (1, heads))
    return (
        values * scale * gain_here * cos_here + swapped * scale * gain_swapped * sin_here
    ).astype(jnp.bfloat16)


def kernel(
    dims,
    q_ref,
    kv_ref,
    disp_ref,
    pick_ref,
    share_ref,
    gate_hbm,
    up_hbm,
    down_hbm,
    mixer_hbm,
    attn_ref,
    moe_ref,
    kv_all,
    incoming,
    hid,
    eo,
    ret,
    att_all,
    gate_w,
    up_w,
    down_w,
    mixer_w,
    m_ref,
    l_ref,
    acc_ref,
    w_sem,
    loc_sem,
    d_send,
    d_recv,
    kv_send,
    kv_recv,
    f_send,
    g_send,
    g_recv,
    h_send,
    h_recv,
    r_send,
    r_recv,
    a_send,
    a_recv,
):
    n, T, head_width, hp = dims
    nz = n // CORES
    e = lax.axis_index("ep")
    t = lax.axis_index("tp")
    z = e // CORES
    c = e % CORES
    sibling = z * CORES + (1 - c)
    kh, rows, pw = q_ref.shape
    keys = kv_ref.shape[1]
    capp = disp_ref.shape[1]
    feat = disp_ref.shape[2]
    ffl = gate_w.shape[1]
    seq = attn_ref.shape[0]

    def offset(k):
        return ((k + 1) // 2) * (2 * (k % 2) - 1)

    def chip(k):
        return (z + offset(k) + 2 * nz) % nz

    def chip_to(k):
        return (z - offset(k) + 2 * nz) % nz

    def rdma(src, dst, ss, rs, axis, index):
        return pltpu.make_async_remote_copy(
            src_ref=src,
            dst_ref=dst,
            send_sem=ss,
            recv_sem=rs,
            device_id={axis: index},
            device_id_type=pl.DeviceIdType.MESH,
        )

    barrier = pltpu.get_barrier_semaphore()

    def greet(j, carry):
        pl.semaphore_signal(
            barrier, inc=1, device_id={"ep": (e + j) % n}, device_id_type=pl.DeviceIdType.MESH
        )
        return carry

    lax.fori_loop(1, n, greet, 0)
    for p in range(1, T):
        pl.semaphore_signal(
            barrier, inc=1, device_id={"tp": (t + p) % T}, device_id_type=pl.DeviceIdType.MESH
        )
    pl.semaphore_wait(barrier, n - 1 + T - 1)

    def d_copy(dest, origin):
        return rdma(
            disp_ref.at[dest], incoming.at[t, origin], d_send.at[dest], d_recv.at[origin], "ep", dest
        )

    def send_disp(k, carry):
        for cc in range(CORES):
            dest = chip_to(k) * CORES + cc

            @pl.when(dest != e)
            def _():
                d_copy(dest, e).start()

        return carry

    lax.fori_loop(0, nz, send_disp, 0)

    def kv_copy(dest, origin, ss):
        src = kv_ref if origin is None else kv_all.at[origin]
        slot = e if origin is None else origin
        return rdma(src, kv_all.at[slot], ss, kv_recv.at[slot], "ep", dest)

    kv_copy(sibling, None, f_send.at[z]).start()

    def send_kv(k, carry):
        zd = chip_to(k)
        kv_copy(zd * CORES + c, None, kv_send.at[zd]).start()
        return carry

    lax.fori_loop(1, nz, send_kv, 0)

    own_disp = pltpu.make_async_copy(disp_ref.at[e], incoming.at[t, e], loc_sem.at[0])
    own_disp.start()
    own_kv = pltpu.make_async_copy(kv_ref, kv_all.at[e], loc_sem.at[1])
    own_kv.start()
    loads = [
        pltpu.make_async_copy(gate_hbm, gate_w, w_sem.at[0]),
        pltpu.make_async_copy(up_hbm, up_w, w_sem.at[1]),
        pltpu.make_async_copy(down_hbm, down_w, w_sem.at[2]),
        pltpu.make_async_copy(mixer_hbm, mixer_w, w_sem.at[3]),
    ]
    for load in loads:
        load.start()
    own_disp.wait()
    own_kv.wait()

    def pair_at(k):
        return pl.ds(chip(k) * CORES, CORES)

    def g_copy(k, owner, peer):
        block = incoming.at[owner, pair_at(k)]
        return rdma(block, block, g_send.at[peer, k], g_recv.at[owner, k], "tp", peer)

    def h_copy(k, owner, peer):
        block = hid.at[owner, pair_at(k)]
        return rdma(block, block, h_send.at[peer, k], h_recv.at[owner, k], "tp", peer)

    def spread(k):
        for cc in range(CORES):
            origin = chip(k) * CORES + cc

            @pl.when(origin != e)
            def _():
                d_copy(origin, origin).wait_recv()

        for p in range(1, T):
            peer = (t + p) % T
            g_copy(k, t, peer).start()

    def attend_block(origin):
        def one_head(h, carry):
            lanes = pl.ds(pl.multiple_of((h * head_width) // pw * pw, pw), pw)
            key_block = kv_all[origin, 0, :, lanes] if kh > 1 else kv_all[origin, 0]
            value_block = kv_all[origin, 1, :, lanes] if kh > 1 else kv_all[origin, 1]
            step = math.gcd(rows, 256)
            for r in range(0, rows, step):
                at = slice(r, r + step)
                scores = lax.dot_general(
                    q_ref[h, at],
                    key_block,
                    (((1,), (1,)), ((), ())),
                    preferred_element_type=jnp.float32,
                )
                old = m_ref[h, at]
                new = jnp.maximum(old, jnp.max(scores, axis=1, keepdims=True))
                weights = jnp.exp(scores - new)
                factor = jnp.exp(old - new)
                m_ref[h, at] = new
                l_ref[h, at] = l_ref[h, at] * factor + jnp.sum(weights, axis=1, keepdims=True)
                acc_ref[h, at] = acc_ref[h, at] * factor + jnp.dot(
                    weights.astype(jnp.bfloat16), value_block, preferred_element_type=jnp.float32
                )
            return carry

        lax.fori_loop(0, kh, one_head, 0)

    def attend(k):
        zk = chip(k)
        mine = zk * CORES + c
        other = zk * CORES + (1 - c)

        @pl.when(k > 0)
        def _():
            kv_copy(mine, mine, kv_send.at[zk]).wait_recv()
            kv_copy(sibling, mine, f_send.at[zk]).start()

        attend_block(mine)
        kv_copy(sibling, other, f_send.at[zk]).wait_recv()
        attend_block(other)

    def first_half(k):
        for p in range(1, T):
            owner = (t + p) % T
            g_copy(k, owner, owner).wait_recv()
        gate = jnp.zeros((CORES * capp, ffl), jnp.float32)
        up = jnp.zeros((CORES * capp, ffl), jnp.float32)
        for s in range(T):
            piece = incoming[s, pair_at(k)].reshape(CORES * capp, feat)
            at = slice(s * feat, (s + 1) * feat)
            gate = gate + jnp.dot(piece, gate_w[at], preferred_element_type=jnp.float32)
            up = up + jnp.dot(piece, up_w[at], preferred_element_type=jnp.float32)
        hidden = (gate / (1.0 + jnp.exp(-gate)) * up).astype(jnp.bfloat16)
        hid[t, pair_at(k)] = hidden.reshape(CORES, capp, ffl)
        for p in range(1, T):
            peer = (t + p) % T
            h_copy(k, t, peer).start()

    def r_copy(dest, origin):
        return rdma(eo.at[dest], ret.at[origin], r_send.at[dest], r_recv.at[origin], "ep", dest)

    def second_half(k):
        for p in range(1, T):
            owner = (t + p) % T
            h_copy(k, owner, owner).wait_recv()
        total = jnp.zeros((CORES * capp, down_w.shape[1]), jnp.float32)
        for s in range(T):
            piece = hid[s, pair_at(k)].reshape(CORES * capp, ffl)
            total = total + jnp.dot(
                piece, down_w[s * ffl : (s + 1) * ffl], preferred_element_type=jnp.float32
            )
        eo[pair_at(k)] = total.astype(jnp.bfloat16).reshape(CORES, capp, down_w.shape[1])
        for cc in range(CORES):
            origin = chip(k) * CORES + cc

            @pl.when(origin != e)
            def _():
                r_copy(origin, e).start()

            @pl.when(origin == e)
            def _():
                ret[origin] = eo[origin]

    m_ref[...] = jnp.full(m_ref.shape, -jnp.inf, jnp.float32)
    l_ref[...] = jnp.zeros(l_ref.shape, jnp.float32)
    acc_ref[...] = jnp.zeros(acc_ref.shape, jnp.float32)

    ahead = min(2, nz)
    for k in range(ahead):
        spread(k)
    loads[0].wait()
    loads[1].wait()
    loads[2].wait()

    def step(k, carry):
        attend(k)
        first_half(k)

        @pl.when(k + ahead < nz)
        def _():
            spread(k + ahead)

        @pl.when(k >= 1)
        def _():
            second_half(k - 1)

        return carry

    lax.fori_loop(0, nz, step, 0)

    group = rows // seq
    for pair in range(kh * head_width // pw):
        heads = []
        for h in range(pair * (pw // head_width), (pair + 1) * (pw // head_width)):
            lane0 = (h * head_width) % pw
            done = acc_ref[h] / l_ref[h]
            for g in range(group):
                heads.append(done[g * seq : (g + 1) * seq, lane0 : lane0 + head_width])
        width = len(heads) * head_width
        att_all[t, :, pair * width : (pair + 1) * width] = jnp.concatenate(heads, axis=1).astype(
            jnp.bfloat16
        )

    def a_copy(owner, peer):
        block = att_all.at[owner]
        return rdma(block, block, a_send.at[peer], a_recv.at[owner], "tp", peer)

    for p in range(1, T):
        a_copy(t, (t + p) % T).start()
    second_half(nz - 1)
    loads[3].wait()
    for p in range(1, T):
        owner = (t + p) % T
        a_copy(owner, owner).wait_recv()
    aw = att_all.shape[2]
    out_cols = attn_ref.shape[1]
    half = math.gcd(out_cols, 256)

    def mix(i, carry):
        at = pl.ds(pl.multiple_of(i * half, half), half)
        total = jnp.zeros((seq, half), jnp.float32)
        for s in range(T):
            total = total + jnp.dot(
                att_all[s], mixer_w[s * aw : (s + 1) * aw, at], preferred_element_type=jnp.float32
            )
        attn_ref[:, at] = total.astype(jnp.bfloat16)
        return carry

    lax.fori_loop(0, out_cols // half, mix, 0)

    def wait_ret(j, carry):
        origin = (e + j) % n
        r_copy(origin, origin).wait_recv()
        return carry

    lax.fori_loop(1, n, wait_ret, 0)
    returned = ret[...].reshape(n * capp, ret.shape[2])
    tokens = moe_ref.shape[0]
    combined = jnp.zeros(moe_ref.shape, jnp.float32)
    for k in range(share_ref.shape[0]):
        combined = combined + share_ref[k] * jnp.dot(
            pick_ref[k], returned, preferred_element_type=jnp.float32
        )
    moe_ref[...] = combined.astype(jnp.bfloat16)

    def drain_ep(j, carry):
        dest = (e + j) % n
        d_copy(dest, e).wait_send()
        r_copy(dest, e).wait_send()
        return carry

    lax.fori_loop(1, n, drain_ep, 0)

    def drain_kv(k, carry):
        zd = chip_to(k)
        kv_copy(zd * CORES + c, None, kv_send.at[zd]).wait_send()
        return carry

    lax.fori_loop(1, nz, drain_kv, 0)

    def drain_tp(k, carry):
        kv_copy(sibling, e, f_send.at[k]).wait_send()
        for p in range(1, T):
            peer = (t + p) % T
            g_copy(k, t, peer).wait_send()
            h_copy(k, t, peer).wait_send()
        return carry

    lax.fori_loop(0, nz, drain_tp, 0)
    for p in range(1, T):
        a_copy(t, (t + p) % T).wait_send()


def on_device(
    n,
    T,
    query_input,
    key_input,
    value_input,
    query_gain,
    key_gain,
    mixer_out,
    moe_input,
    moe_gain,
    routes,
    route_weight,
    expert_gate,
    expert_up,
    expert_down,
):
    seq_dev = query_input.shape[0]
    head_width = query_gain.shape[0]
    heads_here = query_input.shape[1] // head_width
    kh = key_input.shape[1] // head_width
    kw = key_input.shape[1]
    group = heads_here // kh
    pw = min(128, kw)
    hp = pw // head_width
    positions = lax.axis_index("ep") * seq_dev + jnp.arange(seq_dev, dtype=jnp.int32)
    cosine, sine = rope_tables(positions, head_width)
    query_rot = norm_rotate(query_input, query_gain, cosine, sine, head_width)
    key_rot = norm_rotate(key_input, key_gain, cosine, sine, head_width)
    query_rot = query_rot * jnp.bfloat16(head_width ** (-0.5))
    by_head = []
    for h in range(kh):
        for g in range(group):
            col = (h * group + g) * head_width
            place = (h % hp) * head_width
            by_head.append(
                jnp.pad(
                    query_rot[:, col : col + head_width],
                    ((0, 0), (place, pw - head_width - place)),
                )
            )
    q_pad = jnp.stack(by_head).reshape(kh, group * seq_dev, pw)
    key_value = jnp.stack([key_rot, value_input])

    token_count, model_width = moe_input.shape
    top = routes.shape[1]
    local_experts = expert_gate.shape[0]
    assert local_experts == 1
    expert_count = local_experts * n
    capacity = 3 * token_count * top // (2 * expert_count)
    capp = -(-capacity // 16) * 16
    feat = model_width // T
    flat = routes.reshape(-1)
    pairs = token_count * top
    one_hot = flat[:, None] == jnp.arange(expert_count, dtype=jnp.int32)[None, :]
    order = jnp.arange(pairs, dtype=jnp.int32)
    before = (order[:, None] > order[None, :]).astype(jnp.bfloat16)
    earlier = jnp.dot(before, one_hot.astype(jnp.bfloat16), preferred_element_type=jnp.float32)
    slot = jnp.sum(jnp.where(one_hot, earlier, 0.0), axis=1).astype(jnp.int32)
    places = (flat * capp + slot).reshape(token_count, top)
    slots = jnp.arange(n * capp, dtype=jnp.int32)
    pick = (places.T[:, :, None] == slots[None, None, :]).astype(jnp.bfloat16)
    features = moe_input.astype(jnp.float32)
    inv = lax.rsqrt(jnp.mean(features * features, axis=-1, keepdims=True) + epsilon)
    start = lax.axis_index("tp") * feat
    own = lax.dynamic_slice_in_dim(moe_input, start, feat, 1).astype(jnp.float32)
    normed = (own * inv * lax.dynamic_slice_in_dim(moe_gain, start, feat, 0)).astype(jnp.bfloat16)
    disp = lax.dot_general(
        jnp.sum(pick, axis=0),
        normed,
        (((0,), (0,)), ((), ())),
        preferred_element_type=jnp.float32,
    ).astype(jnp.bfloat16)
    disp = disp.reshape(n, capp, feat)
    shares = route_weight / jnp.sum(route_weight, axis=-1, keepdims=True)
    shares = shares.T[:, :, None]

    gate = expert_gate[0]
    up = expert_up[0]
    down = expert_down[0]
    ffl = gate.shape[1]
    cols = down.shape[1]
    nz = n // CORES
    aw = heads_here * head_width
    out_cols = mixer_out.shape[1]
    bf = jnp.bfloat16
    dma = pltpu.SemaphoreType.DMA
    vmem = pl.BlockSpec(memory_space=pltpu.VMEM)
    hbm = pl.BlockSpec(memory_space=pl.ANY)
    return pl.pallas_call(
        functools.partial(kernel, (n, T, head_width, hp)),
        out_shape=(
            jax.ShapeDtypeStruct((seq_dev, out_cols), bf),
            jax.ShapeDtypeStruct((token_count, cols), bf),
        ),
        in_specs=[vmem] * 5 + [hbm] * 4,
        out_specs=(vmem, vmem),
        scratch_shapes=[
            pltpu.VMEM((n, 2, seq_dev, kw), bf),
            pltpu.VMEM((T, n, capp, feat), bf),
            pltpu.VMEM((T, n, capp, ffl), bf),
            pltpu.VMEM((n, capp, cols), bf),
            pltpu.VMEM((n, capp, cols), bf),
            pltpu.VMEM((T, seq_dev, aw), bf),
            pltpu.VMEM(gate.shape, bf),
            pltpu.VMEM(up.shape, bf),
            pltpu.VMEM(down.shape, bf),
            pltpu.VMEM(mixer_out.shape, bf),
            pltpu.VMEM((kh, group * seq_dev, 1), jnp.float32),
            pltpu.VMEM((kh, group * seq_dev, 1), jnp.float32),
            pltpu.VMEM((kh, group * seq_dev, pw), jnp.float32),
            dma((4,)),
            dma((2,)),
            dma((n,)),
            dma((n,)),
            dma((nz,)),
            dma((n,)),
            dma((nz,)),
            dma((T, nz)),
            dma((T, nz)),
            dma((T, nz)),
            dma((T, nz)),
            dma((n,)),
            dma((n,)),
            dma((T,)),
            dma((T,)),
        ],
        compiler_params=pltpu.CompilerParams(
            collective_id=0, has_side_effects=True, vmem_limit_bytes=63 * 1024 * 1024
        ),
    )(q_pad, key_value, disp, pick, shares, gate, up, down, mixer_out)


def solution(mesh):
    placed = (
        P("ep", "tp"),
        P("ep", "tp"),
        P("ep", "tp"),
        P(),
        P(),
        P(None, "tp"),
        P("ep", None),
        P(),
        P("ep", None),
        P("ep", None),
        P("ep", None, "tp"),
        P("ep", None, "tp"),
        P("ep", None, "tp"),
    )
    return jax.shard_map(
        functools.partial(on_device, mesh.shape["ep"], mesh.shape["tp"]),
        mesh=mesh,
        in_specs=placed,
        out_specs=(P("ep", "tp"), P("ep", "tp")),
        check_vma=False,
    )
```

```python
import functools
import math

import jax
import jax.numpy as jnp
from jax import lax
from jax.experimental import pallas as pl
from jax.experimental.pallas import tpu as pltpu
from jax.sharding import PartitionSpec as P

GRID_W = 64
CORES = 2

epsilon = 1e-06
base_theta = 10000.0


def rope_tables(positions, head_width):
    quarter = head_width // 4
    inverse = base_theta ** (-jnp.arange(quarter, dtype=jnp.float32) / quarter)
    grid_row = (positions // GRID_W).astype(jnp.float32)
    grid_col = (positions % GRID_W).astype(jnp.float32)
    angles = jnp.concatenate(
        [grid_row[:, None] * inverse[None, :], grid_col[:, None] * inverse[None, :]], axis=1
    )
    return (jnp.cos(angles), jnp.sin(angles))


def norm_rotate(columns, gain, cosine, sine, head_width):
    width = columns.shape[1]
    heads = width // head_width
    lane = jnp.arange(width)
    same_head = (lane[:, None] // head_width == lane[None, :] // head_width).astype(jnp.float32)
    half = head_width // 2
    within = lane % head_width
    partner = jnp.where(within < half, lane + half, lane - half)
    swap = (lane[:, None] == partner[None, :]).astype(jnp.bfloat16)
    values = columns.astype(jnp.float32)
    mean = (
        jnp.dot(values * values, same_head, precision=lax.Precision.HIGHEST) / head_width
    )
    scale = lax.rsqrt(mean + epsilon)
    swapped = jnp.dot(columns, swap, preferred_element_type=jnp.float32)
    gain_here = jnp.tile(gain, heads)[None, :]
    gain_swapped = jnp.tile(jnp.roll(gain, half), heads)[None, :]
    cos_here = jnp.tile(cosine, (1, 2 * heads))
    sin_here = jnp.tile(jnp.concatenate([-sine, sine], axis=1), (1, heads))
    return (
        values * scale * gain_here * cos_here + swapped * scale * gain_swapped * sin_here
    ).astype(jnp.bfloat16)


def kernel(
    dims,
    q_ref,
    kv_ref,
    disp_ref,
    near_ref,
    pick_ref,
    share_ref,
    gate_hbm,
    up_hbm,
    down_hbm,
    mixer_hbm,
    attn_ref,
    moe_ref,
    kv_all,
    incoming,
    hid,
    eo,
    ret,
    att_all,
    gate_w,
    up_w,
    down_w,
    mixer_w,
    m_ref,
    l_ref,
    acc_ref,
    w_sem,
    loc_sem,
    d_send,
    d_recv,
    kv_send,
    kv_recv,
    f_send,
    g_send,
    g_recv,
    h_send,
    h_recv,
    r_send,
    r_recv,
    a_send,
    a_recv,
    gf_send,
    gf_recv,
    af_send,
    af_recv,
):
    n, T, head_width, hp = dims
    nz = n // CORES
    e = lax.axis_index("ep")
    t = lax.axis_index("tp")
    z = e // CORES
    c = e % CORES
    sibling = z * CORES + (1 - c)
    kh, rows, pw = q_ref.shape
    keys = kv_ref.shape[1]
    capp = disp_ref.shape[1]
    feat = disp_ref.shape[2]
    ffl = gate_w.shape[1]
    seq = attn_ref.shape[0]
    square = T == 4
    x_peer = (t // 2) * 2 + 1 - t % 2
    y_peer = (1 - t // 2) * 2 + t % 2
    far_peer = 3 - t
    peers = [x_peer, y_peer] if square else [(t + p) % T for p in range(1, T)]

    def offset(k):
        return ((k + 1) // 2) * (2 * (k % 2) - 1)

    def chip(k):
        return (z + offset(k) + 2 * nz) % nz

    def chip_to(k):
        return (z - offset(k) + 2 * nz) % nz

    def rdma(src, dst, ss, rs, axis, index):
        return pltpu.make_async_remote_copy(
            src_ref=src,
            dst_ref=dst,
            send_sem=ss,
            recv_sem=rs,
            device_id={axis: index},
            device_id_type=pl.DeviceIdType.MESH,
        )

    barrier = pltpu.get_barrier_semaphore()

    def greet(j, carry):
        pl.semaphore_signal(
            barrier, inc=1, device_id={"ep": (e + j) % n}, device_id_type=pl.DeviceIdType.MESH
        )
        return carry

    lax.fori_loop(1, n, greet, 0)
    for p in range(1, T):
        pl.semaphore_signal(
            barrier, inc=1, device_id={"tp": (t + p) % T}, device_id_type=pl.DeviceIdType.MESH
        )
    pl.semaphore_wait(barrier, n - 1 + T - 1)

    def d_copy(dest, origin):
        return rdma(
            disp_ref.at[dest], incoming.at[t, origin], d_send.at[dest], d_recv.at[origin], "ep", dest
        )

    def near_copy(origin):
        return rdma(
            near_ref.at[1 - c],
            incoming.at[:, origin],
            d_send.at[sibling],
            d_recv.at[origin],
            "ep",
            sibling,
        )

    near_copy(e).start()

    def send_disp(k, carry):
        for cc in range(CORES):
            d_copy(chip_to(k) * CORES + cc, e).start()
        return carry

    lax.fori_loop(1, nz, send_disp, 0)

    def kv_copy(dest, origin, ss):
        src = kv_ref if origin is None else kv_all.at[origin]
        slot = e if origin is None else origin
        return rdma(src, kv_all.at[slot], ss, kv_recv.at[slot], "ep", dest)

    kv_copy(sibling, None, f_send.at[z]).start()

    def send_kv(k, carry):
        zd = chip_to(k)
        kv_copy(zd * CORES + c, None, kv_send.at[zd]).start()
        return carry

    lax.fori_loop(1, nz, send_kv, 0)

    own_disp = pltpu.make_async_copy(near_ref.at[c], incoming.at[:, e], loc_sem.at[0])
    own_disp.start()
    own_kv = pltpu.make_async_copy(kv_ref, kv_all.at[e], loc_sem.at[1])
    own_kv.start()
    loads = [
        pltpu.make_async_copy(gate_hbm, gate_w, w_sem.at[0]),
        pltpu.make_async_copy(up_hbm, up_w, w_sem.at[1]),
        pltpu.make_async_copy(down_hbm, down_w, w_sem.at[2]),
        pltpu.make_async_copy(mixer_hbm, mixer_w, w_sem.at[3]),
    ]
    for load in loads:
        load.start()
    own_disp.wait()
    own_kv.wait()

    def pair_at(k):
        return pl.ds(chip(k) * CORES, CORES)

    def g_copy(k, owner, peer):
        block = incoming.at[owner, pair_at(k)]
        return rdma(block, block, g_send.at[peer, k], g_recv.at[owner, k], "tp", peer)

    def h_copy(k, owner, peer):
        block = hid.at[owner, pair_at(k)]
        return rdma(block, block, h_send.at[peer, k], h_recv.at[owner, k], "tp", peer)

    def spread(k):
        for cc in range(CORES):
            origin = chip(k) * CORES + cc
            d_copy(origin, origin).wait_recv()
        for peer in peers:
            g_copy(k, t, peer).start()

    def g_relay(k, owner, cc, peer):
        block = incoming.at[owner, chip(k) * CORES + cc]
        return rdma(block, block, gf_send.at[cc, k], gf_recv.at[cc, k], "tp", peer)

    def relay(k):
        for owner in peers:
            g_copy(k, owner, owner).wait_recv()
        if square:
            g_relay(k, x_peer, 0, y_peer).start()
            g_relay(k, y_peer, 1, x_peer).start()

    def relayed(k):
        if square:
            g_relay(k, far_peer, 0, y_peer).wait_recv()
            g_relay(k, far_peer, 1, x_peer).wait_recv()

    def attend_block(origin):
        def one_head(h, carry):
            lanes = pl.ds(pl.multiple_of((h * head_width) // pw * pw, pw), pw)
            key_block = kv_all[origin, 0, :, lanes] if kh > 1 else kv_all[origin, 0]
            value_block = kv_all[origin, 1, :, lanes] if kh > 1 else kv_all[origin, 1]
            step = math.gcd(rows, 256)
            for r in range(0, rows, step):
                at = slice(r, r + step)
                scores = lax.dot_general(
                    q_ref[h, at],
                    key_block,
                    (((1,), (1,)), ((), ())),
                    preferred_element_type=jnp.float32,
                )
                old = m_ref[h, at]
                new = jnp.maximum(old, jnp.max(scores, axis=1, keepdims=True))
                weights = jnp.exp(scores - new)
                factor = jnp.exp(old - new)
                m_ref[h, at] = new
                l_ref[h, at] = l_ref[h, at] * factor + jnp.sum(weights, axis=1, keepdims=True)
                acc_ref[h, at] = acc_ref[h, at] * factor + jnp.dot(
                    weights.astype(jnp.bfloat16), value_block, preferred_element_type=jnp.float32
                )
            return carry

        lax.fori_loop(0, kh, one_head, 0)

    def attend(k):
        zk = chip(k)
        mine = zk * CORES + c
        other = zk * CORES + (1 - c)

        kv_copy(mine, mine, kv_send.at[zk]).wait_recv()
        kv_copy(sibling, mine, f_send.at[zk]).start()
        attend_block(mine)
        kv_copy(sibling, other, f_send.at[zk]).wait_recv()
        attend_block(other)

    def first_half(k):
        gate = jnp.zeros((CORES * capp, ffl), jnp.float32)
        up = jnp.zeros((CORES * capp, ffl), jnp.float32)
        for s in range(T):
            piece = incoming[s, pair_at(k)].reshape(CORES * capp, feat)
            at = slice(s * feat, (s + 1) * feat)
            gate = gate + jnp.dot(piece, gate_w[at], preferred_element_type=jnp.float32)
            up = up + jnp.dot(piece, up_w[at], preferred_element_type=jnp.float32)
        hidden = (gate / (1.0 + jnp.exp(-gate)) * up).astype(jnp.bfloat16)
        hid[t, pair_at(k)] = hidden.reshape(CORES, capp, ffl)
        for p in range(1, T):
            peer = (t + p) % T
            h_copy(k, t, peer).start()

    def r_copy(dest, origin):
        return rdma(eo.at[dest], ret.at[origin], r_send.at[dest], r_recv.at[origin], "ep", dest)

    def second_half(k):
        for p in range(1, T):
            owner = (t + p) % T
            h_copy(k, owner, owner).wait_recv()
        total = jnp.zeros((CORES * capp, down_w.shape[1]), jnp.float32)
        for s in range(T):
            piece = hid[s, pair_at(k)].reshape(CORES * capp, ffl)
            total = total + jnp.dot(
                piece, down_w[s * ffl : (s + 1) * ffl], preferred_element_type=jnp.float32
            )
        eo[pair_at(k)] = total.astype(jnp.bfloat16).reshape(CORES, capp, down_w.shape[1])
        for cc in range(CORES):
            origin = chip(k) * CORES + cc

            @pl.when(origin != e)
            def _():
                r_copy(origin, e).start()

            @pl.when(origin == e)
            def _():
                ret[origin] = eo[origin]

    m_ref[...] = jnp.full(m_ref.shape, -jnp.inf, jnp.float32)
    l_ref[...] = jnp.zeros(l_ref.shape, jnp.float32)
    acc_ref[...] = jnp.zeros(acc_ref.shape, jnp.float32)

    attend_block(e)
    near_copy(sibling).wait_recv()
    loads[0].wait()
    loads[1].wait()
    loads[2].wait()
    first_half(0)
    if nz > 1:
        spread(1)
    kv_copy(sibling, sibling, f_send.at[z]).wait_recv()
    attend_block(sibling)

    def step(k, carry):
        @pl.when(k + 1 < nz)
        def _():
            spread(k + 1)

        relay(k)
        attend(k)
        relayed(k)
        first_half(k)
        second_half(k - 1)
        return carry

    lax.fori_loop(1, nz, step, 0)

    group = rows // seq
    for pair in range(kh * head_width // pw):
        heads = []
        for h in range(pair * (pw // head_width), (pair + 1) * (pw // head_width)):
            lane0 = (h * head_width) % pw
            done = acc_ref[h] / l_ref[h]
            for g in range(group):
                heads.append(done[g * seq : (g + 1) * seq, lane0 : lane0 + head_width])
        width = len(heads) * head_width
        att_all[t, :, pair * width : (pair + 1) * width] = jnp.concatenate(heads, axis=1).astype(
            jnp.bfloat16
        )

    def a_copy(owner, peer):
        block = att_all.at[owner]
        return rdma(block, block, a_send.at[peer], a_recv.at[owner], "tp", peer)

    def a_relay(owner, part, peer):
        block = att_all.at[owner, pl.ds(part * (seq // 2), seq // 2)]
        return rdma(block, block, af_send.at[part], af_recv.at[part], "tp", peer)

    for peer in peers:
        a_copy(t, peer).start()
    second_half(nz - 1)
    loads[3].wait()
    for owner in peers:
        a_copy(owner, owner).wait_recv()
    if square:
        a_relay(x_peer, 0, y_peer).start()
        a_relay(y_peer, 1, x_peer).start()
        a_relay(far_peer, 0, y_peer).wait_recv()
        a_relay(far_peer, 1, x_peer).wait_recv()
    aw = att_all.shape[2]
    out_cols = attn_ref.shape[1]
    half = math.gcd(out_cols, 256)

    def mix(i, carry):
        at = pl.ds(pl.multiple_of(i * half, half), half)
        total = jnp.zeros((seq, half), jnp.float32)
        for s in range(T):
            total = total + jnp.dot(
                att_all[s], mixer_w[s * aw : (s + 1) * aw, at], preferred_element_type=jnp.float32
            )
        attn_ref[:, at] = total.astype(jnp.bfloat16)
        return carry

    lax.fori_loop(0, out_cols // half, mix, 0)

    def wait_ret(j, carry):
        origin = (e + j) % n
        r_copy(origin, origin).wait_recv()
        return carry

    lax.fori_loop(1, n, wait_ret, 0)
    returned = ret[...].reshape(n * capp, ret.shape[2])
    tokens = moe_ref.shape[0]
    combined = jnp.zeros(moe_ref.shape, jnp.float32)
    for k in range(share_ref.shape[0]):
        combined = combined + share_ref[k] * jnp.dot(
            pick_ref[k], returned, preferred_element_type=jnp.float32
        )
    moe_ref[...] = combined.astype(jnp.bfloat16)

    def drain_ep(j, carry):
        dest = (e + j) % n
        r_copy(dest, e).wait_send()
        return carry

    lax.fori_loop(1, n, drain_ep, 0)
    near_copy(e).wait_send()

    def drain_kv(k, carry):
        zd = chip_to(k)
        kv_copy(zd * CORES + c, None, kv_send.at[zd]).wait_send()
        for cc in range(CORES):
            d_copy(zd * CORES + cc, e).wait_send()
        for peer in peers:
            g_copy(k, t, peer).wait_send()
        if square:
            g_relay(k, x_peer, 0, y_peer).wait_send()
            g_relay(k, y_peer, 1, x_peer).wait_send()
        return carry

    lax.fori_loop(1, nz, drain_kv, 0)

    def drain_tp(k, carry):
        kv_copy(sibling, e, f_send.at[k]).wait_send()
        for p in range(1, T):
            h_copy(k, t, (t + p) % T).wait_send()
        return carry

    lax.fori_loop(0, nz, drain_tp, 0)
    for peer in peers:
        a_copy(t, peer).wait_send()
    if square:
        a_relay(x_peer, 0, y_peer).wait_send()
        a_relay(y_peer, 1, x_peer).wait_send()


def on_device(
    n,
    T,
    query_input,
    key_input,
    value_input,
    query_gain,
    key_gain,
    mixer_out,
    moe_input,
    moe_gain,
    routes,
    route_weight,
    expert_gate,
    expert_up,
    expert_down,
):
    seq_dev = query_input.shape[0]
    head_width = query_gain.shape[0]
    heads_here = query_input.shape[1] // head_width
    kh = key_input.shape[1] // head_width
    kw = key_input.shape[1]
    group = heads_here // kh
    pw = min(128, kw)
    hp = pw // head_width
    positions = lax.axis_index("ep") * seq_dev + jnp.arange(seq_dev, dtype=jnp.int32)
    cosine, sine = rope_tables(positions, head_width)
    query_rot = norm_rotate(query_input, query_gain, cosine, sine, head_width)
    key_rot = norm_rotate(key_input, key_gain, cosine, sine, head_width)
    query_rot = query_rot * jnp.bfloat16(head_width ** (-0.5))
    by_head = []
    for h in range(kh):
        for g in range(group):
            col = (h * group + g) * head_width
            place = (h % hp) * head_width
            by_head.append(
                jnp.pad(
                    query_rot[:, col : col + head_width],
                    ((0, 0), (place, pw - head_width - place)),
                )
            )
    q_pad = jnp.stack(by_head).reshape(kh, group * seq_dev, pw)
    key_value = jnp.stack([key_rot, value_input])

    token_count, model_width = moe_input.shape
    top = routes.shape[1]
    local_experts = expert_gate.shape[0]
    assert local_experts == 1
    expert_count = local_experts * n
    capacity = 3 * token_count * top // (2 * expert_count)
    capp = -(-capacity // 16) * 16
    feat = model_width // T
    flat = routes.reshape(-1)
    pairs = token_count * top
    one_hot = flat[:, None] == jnp.arange(expert_count, dtype=jnp.int32)[None, :]
    order = jnp.arange(pairs, dtype=jnp.int32)
    before = (order[:, None] > order[None, :]).astype(jnp.bfloat16)
    earlier = jnp.dot(before, one_hot.astype(jnp.bfloat16), preferred_element_type=jnp.float32)
    slot = jnp.sum(jnp.where(one_hot, earlier, 0.0), axis=1).astype(jnp.int32)
    places = (flat * capp + slot).reshape(token_count, top)
    slots = jnp.arange(n * capp, dtype=jnp.int32)
    pick = (places.T[:, :, None] == slots[None, None, :]).astype(jnp.bfloat16)
    features = moe_input.astype(jnp.float32)
    inv = lax.rsqrt(jnp.mean(features * features, axis=-1, keepdims=True) + epsilon)
    normed = (features * inv * moe_gain).astype(jnp.bfloat16)
    own = lax.dynamic_slice_in_dim(normed, lax.axis_index("tp") * feat, feat, 1)
    sent = jnp.sum(pick, axis=0)
    disp = lax.dot_general(
        sent, own, (((0,), (0,)), ((), ())), preferred_element_type=jnp.float32
    ).astype(jnp.bfloat16)
    disp = disp.reshape(n, capp, feat)
    here = (lax.axis_index("ep") // CORES) * CORES * capp
    near_sent = lax.dynamic_slice_in_dim(sent, here, CORES * capp, 1)
    near = lax.dot_general(
        near_sent, normed, (((0,), (0,)), ((), ())), preferred_element_type=jnp.float32
    ).astype(jnp.bfloat16)
    near = jnp.transpose(near.reshape(CORES, capp, T, feat), (0, 2, 1, 3))
    shares = route_weight / jnp.sum(route_weight, axis=-1, keepdims=True)
    shares = shares.T[:, :, None]

    gate = expert_gate[0]
    up = expert_up[0]
    down = expert_down[0]
    ffl = gate.shape[1]
    cols = down.shape[1]
    nz = n // CORES
    aw = heads_here * head_width
    out_cols = mixer_out.shape[1]
    bf = jnp.bfloat16
    dma = pltpu.SemaphoreType.DMA
    vmem = pl.BlockSpec(memory_space=pltpu.VMEM)
    hbm = pl.BlockSpec(memory_space=pl.ANY)
    return pl.pallas_call(
        functools.partial(kernel, (n, T, head_width, hp)),
        out_shape=(
            jax.ShapeDtypeStruct((seq_dev, out_cols), bf),
            jax.ShapeDtypeStruct((token_count, cols), bf),
        ),
        in_specs=[vmem] * 6 + [hbm] * 4,
        out_specs=(vmem, vmem),
        scratch_shapes=[
            pltpu.VMEM((n, 2, seq_dev, kw), bf),
            pltpu.VMEM((T, n, capp, feat), bf),
            pltpu.VMEM((T, n, capp, ffl), bf),
            pltpu.VMEM((n, capp, cols), bf),
            pltpu.VMEM((n, capp, cols), bf),
            pltpu.VMEM((T, seq_dev, aw), bf),
            pltpu.VMEM(gate.shape, bf),
            pltpu.VMEM(up.shape, bf),
            pltpu.VMEM(down.shape, bf),
            pltpu.VMEM(mixer_out.shape, bf),
            pltpu.VMEM((kh, group * seq_dev, 1), jnp.float32),
            pltpu.VMEM((kh, group * seq_dev, 1), jnp.float32),
            pltpu.VMEM((kh, group * seq_dev, pw), jnp.float32),
            dma((4,)),
            dma((2,)),
            dma((n,)),
            dma((n,)),
            dma((nz,)),
            dma((n,)),
            dma((nz,)),
            dma((T, nz)),
            dma((T, nz)),
            dma((T, nz)),
            dma((T, nz)),
            dma((n,)),
            dma((n,)),
            dma((T,)),
            dma((T,)),
            dma((2, nz)),
            dma((2, nz)),
            dma((2,)),
            dma((2,)),
        ],
        compiler_params=pltpu.CompilerParams(
            collective_id=0, has_side_effects=True, vmem_limit_bytes=63 * 1024 * 1024
        ),
    )(q_pad, key_value, disp, near, pick, shares, gate, up, down, mixer_out)


def solution(mesh):
    placed = (
        P("ep", "tp"),
        P("ep", "tp"),
        P("ep", "tp"),
        P(),
        P(),
        P(None, "tp"),
        P("ep", None),
        P(),
        P("ep", None),
        P("ep", None),
        P("ep", None, "tp"),
        P("ep", None, "tp"),
        P("ep", None, "tp"),
    )
    return jax.shard_map(
        functools.partial(on_device, mesh.shape["ep"], mesh.shape["tp"]),
        mesh=mesh,
        in_specs=placed,
        out_specs=(P("ep", "tp"), P("ep", "tp")),
        check_vma=False,
    )
```

```python
import functools
import math

import jax
import jax.numpy as jnp
from jax import lax
from jax.experimental import pallas as pl
from jax.experimental.pallas import tpu as pltpu
from jax.sharding import PartitionSpec as P

GRID_W = 64
CORES = 2

epsilon = 1e-06
base_theta = 10000.0


def rope_tables(positions, head_width):
    quarter = head_width // 4
    inverse = base_theta ** (-jnp.arange(quarter, dtype=jnp.float32) / quarter)
    grid_row = (positions // GRID_W).astype(jnp.float32)
    grid_col = (positions % GRID_W).astype(jnp.float32)
    angles = jnp.concatenate(
        [grid_row[:, None] * inverse[None, :], grid_col[:, None] * inverse[None, :]], axis=1
    )
    return (jnp.cos(angles), jnp.sin(angles))


def norm_rotate(columns, gain, cosine, sine, head_width):
    width = columns.shape[1]
    heads = width // head_width
    lane = jnp.arange(width)
    same_head = (lane[:, None] // head_width == lane[None, :] // head_width).astype(jnp.float32)
    half = head_width // 2
    within = lane % head_width
    partner = jnp.where(within < half, lane + half, lane - half)
    swap = (lane[:, None] == partner[None, :]).astype(jnp.bfloat16)
    values = columns.astype(jnp.float32)
    mean = (
        jnp.dot(values * values, same_head, precision=lax.Precision.HIGHEST) / head_width
    )
    scale = lax.rsqrt(mean + epsilon)
    swapped = jnp.dot(columns, swap, preferred_element_type=jnp.float32)
    gain_here = jnp.tile(gain, heads)[None, :]
    gain_swapped = jnp.tile(jnp.roll(gain, half), heads)[None, :]
    cos_here = jnp.tile(cosine, (1, 2 * heads))
    sin_here = jnp.tile(jnp.concatenate([-sine, sine], axis=1), (1, heads))
    return (
        values * scale * gain_here * cos_here + swapped * scale * gain_swapped * sin_here
    ).astype(jnp.bfloat16)


def kernel(
    dims,
    q_ref,
    kv_ref,
    disp_ref,
    pick_ref,
    share_ref,
    gate_hbm,
    up_hbm,
    down_hbm,
    mixer_hbm,
    attn_ref,
    moe_ref,
    kv_all,
    incoming,
    hid,
    eo,
    ret,
    att_all,
    gate_w,
    up_w,
    down_w,
    mixer_w,
    m_ref,
    l_ref,
    acc_ref,
    w_sem,
    loc_sem,
    d_send,
    d_recv,
    kv_send,
    kv_recv,
    f_send,
    g_send,
    g_recv,
    h_send,
    h_recv,
    r_send,
    r_recv,
    a_send,
    a_recv,
    gf_send,
    gf_recv,
    af_send,
    af_recv,
):
    n, T, head_width, hp = dims
    nz = n // CORES
    e = lax.axis_index("ep")
    t = lax.axis_index("tp")
    z = e // CORES
    c = e % CORES
    sibling = z * CORES + (1 - c)
    kh, rows, pw = q_ref.shape
    keys = kv_ref.shape[1]
    capp = disp_ref.shape[1]
    feat = disp_ref.shape[2]
    ffl = gate_w.shape[1]
    seq = attn_ref.shape[0]
    square = T == 4
    x_peer = (t // 2) * 2 + 1 - t % 2
    y_peer = (1 - t // 2) * 2 + t % 2
    far_peer = 3 - t
    peers = [x_peer, y_peer] if square else [(t + p) % T for p in range(1, T)]

    def offset(k):
        return ((k + 1) // 2) * (2 * (k % 2) - 1)

    def chip(k):
        return (z + offset(k) + 2 * nz) % nz

    def chip_to(k):
        return (z - offset(k) + 2 * nz) % nz

    def rdma(src, dst, ss, rs, axis, index):
        return pltpu.make_async_remote_copy(
            src_ref=src,
            dst_ref=dst,
            send_sem=ss,
            recv_sem=rs,
            device_id={axis: index},
            device_id_type=pl.DeviceIdType.MESH,
        )

    barrier = pltpu.get_barrier_semaphore()

    def greet(j, carry):
        pl.semaphore_signal(
            barrier, inc=1, device_id={"ep": (e + j) % n}, device_id_type=pl.DeviceIdType.MESH
        )
        return carry

    lax.fori_loop(1, n, greet, 0)
    for p in range(1, T):
        pl.semaphore_signal(
            barrier, inc=1, device_id={"tp": (t + p) % T}, device_id_type=pl.DeviceIdType.MESH
        )
    pl.semaphore_wait(barrier, n - 1 + T - 1)

    def d_copy(dest, origin):
        return rdma(
            disp_ref.at[dest], incoming.at[t, origin], d_send.at[dest], d_recv.at[origin], "ep", dest
        )

    def send_disp(k, carry):
        for cc in range(CORES):
            dest = chip_to(k) * CORES + cc

            @pl.when(dest != e)
            def _():
                d_copy(dest, e).start()

        return carry

    lax.fori_loop(0, nz, send_disp, 0)

    def kv_copy(dest, origin, ss):
        src = kv_ref if origin is None else kv_all.at[origin]
        slot = e if origin is None else origin
        return rdma(src, kv_all.at[slot], ss, kv_recv.at[slot], "ep", dest)

    kv_copy(sibling, None, f_send.at[z]).start()

    def send_kv(k, carry):
        zd = chip_to(k)
        kv_copy(zd * CORES + c, None, kv_send.at[zd]).start()
        return carry

    lax.fori_loop(1, nz, send_kv, 0)

    own_disp = pltpu.make_async_copy(disp_ref.at[e], incoming.at[t, e], loc_sem.at[0])
    own_disp.start()
    own_kv = pltpu.make_async_copy(kv_ref, kv_all.at[e], loc_sem.at[1])
    own_kv.start()
    loads = [
        pltpu.make_async_copy(gate_hbm, gate_w, w_sem.at[0]),
        pltpu.make_async_copy(up_hbm, up_w, w_sem.at[1]),
        pltpu.make_async_copy(down_hbm, down_w, w_sem.at[2]),
        pltpu.make_async_copy(mixer_hbm, mixer_w, w_sem.at[3]),
    ]
    for load in loads:
        load.start()
    own_disp.wait()
    own_kv.wait()

    def pair_at(k):
        return pl.ds(chip(k) * CORES, CORES)

    def g_copy(k, owner, peer):
        block = incoming.at[owner, pair_at(k)]
        return rdma(block, block, g_send.at[peer, k], g_recv.at[owner, k], "tp", peer)

    def h_copy(k, owner, peer):
        block = hid.at[owner, pair_at(k)]
        return rdma(block, block, h_send.at[peer, k], h_recv.at[owner, k], "tp", peer)

    def spread(k):
        for cc in range(CORES):
            origin = chip(k) * CORES + cc

            @pl.when(origin != e)
            def _():
                d_copy(origin, origin).wait_recv()

        for peer in peers:
            g_copy(k, t, peer).start()

    def g_relay(k, owner, cc, peer):
        block = incoming.at[owner, chip(k) * CORES + cc]
        return rdma(block, block, gf_send.at[cc, k], gf_recv.at[cc, k], "tp", peer)

    def relay(k):
        for owner in peers:
            g_copy(k, owner, owner).wait_recv()
        if square:
            g_relay(k, x_peer, 0, y_peer).start()
            g_relay(k, y_peer, 1, x_peer).start()

    def relayed(k):
        if square:
            g_relay(k, far_peer, 0, y_peer).wait_recv()
            g_relay(k, far_peer, 1, x_peer).wait_recv()

    def attend_block(origin):
        def one_head(h, carry):
            lanes = pl.ds(pl.multiple_of((h * head_width) // pw * pw, pw), pw)
            key_block = kv_all[origin, 0, :, lanes] if kh > 1 else kv_all[origin, 0]
            value_block = kv_all[origin, 1, :, lanes] if kh > 1 else kv_all[origin, 1]
            step = math.gcd(rows, 256)
            for r in range(0, rows, step):
                at = slice(r, r + step)
                scores = lax.dot_general(
                    q_ref[h, at],
                    key_block,
                    (((1,), (1,)), ((), ())),
                    preferred_element_type=jnp.float32,
                )
                old = m_ref[h, at]
                new = jnp.maximum(old, jnp.max(scores, axis=1, keepdims=True))
                weights = jnp.exp(scores - new)
                factor = jnp.exp(old - new)
                m_ref[h, at] = new
                l_ref[h, at] = l_ref[h, at] * factor + jnp.sum(weights, axis=1, keepdims=True)
                acc_ref[h, at] = acc_ref[h, at] * factor + jnp.dot(
                    weights.astype(jnp.bfloat16), value_block, preferred_element_type=jnp.float32
                )
            return carry

        lax.fori_loop(0, kh, one_head, 0)

    def attend(k):
        zk = chip(k)
        mine = zk * CORES + c
        other = zk * CORES + (1 - c)

        kv_copy(mine, mine, kv_send.at[zk]).wait_recv()
        kv_copy(sibling, mine, f_send.at[zk]).start()
        attend_block(mine)
        kv_copy(sibling, other, f_send.at[zk]).wait_recv()
        attend_block(other)

    def first_half(k):
        gate = jnp.zeros((CORES * capp, ffl), jnp.float32)
        up = jnp.zeros((CORES * capp, ffl), jnp.float32)
        for s in range(T):
            piece = incoming[s, pair_at(k)].reshape(CORES * capp, feat)
            at = slice(s * feat, (s + 1) * feat)
            gate = gate + jnp.dot(piece, gate_w[at], preferred_element_type=jnp.float32)
            up = up + jnp.dot(piece, up_w[at], preferred_element_type=jnp.float32)
        hidden = (gate / (1.0 + jnp.exp(-gate)) * up).astype(jnp.bfloat16)
        hid[t, pair_at(k)] = hidden.reshape(CORES, capp, ffl)
        for p in range(1, T):
            peer = (t + p) % T
            h_copy(k, t, peer).start()

    def r_copy(dest, origin):
        return rdma(eo.at[dest], ret.at[origin], r_send.at[dest], r_recv.at[origin], "ep", dest)

    def second_half(k):
        for p in range(1, T):
            owner = (t + p) % T
            h_copy(k, owner, owner).wait_recv()
        total = jnp.zeros((CORES * capp, down_w.shape[1]), jnp.float32)
        for s in range(T):
            piece = hid[s, pair_at(k)].reshape(CORES * capp, ffl)
            total = total + jnp.dot(
                piece, down_w[s * ffl : (s + 1) * ffl], preferred_element_type=jnp.float32
            )
        eo[pair_at(k)] = total.astype(jnp.bfloat16).reshape(CORES, capp, down_w.shape[1])
        for cc in range(CORES):
            origin = chip(k) * CORES + cc

            @pl.when(origin != e)
            def _():
                r_copy(origin, e).start()

            @pl.when(origin == e)
            def _():
                ret[origin] = eo[origin]

    m_ref[...] = jnp.full(m_ref.shape, -jnp.inf, jnp.float32)
    l_ref[...] = jnp.zeros(l_ref.shape, jnp.float32)
    acc_ref[...] = jnp.zeros(acc_ref.shape, jnp.float32)

    spread(0)
    attend_block(e)
    relay(0)
    for load in loads[:3]:
        load.wait()
    if nz > 1:
        spread(1)
    relayed(0)
    first_half(0)
    kv_copy(sibling, sibling, f_send.at[z]).wait_recv()
    attend_block(sibling)

    def step(k, carry):
        @pl.when(k + 1 < nz)
        def _():
            spread(k + 1)

        relay(k)
        second_half(k - 1)
        relayed(k)
        first_half(k)

        @pl.when(k >= 2)
        def _():
            attend(k - 1)

        return carry

    lax.fori_loop(1, nz, step, 0)
    second_half(nz - 1)
    if nz > 1:
        attend(nz - 1)

    group = rows // seq
    for pair in range(kh * head_width // pw):
        heads = []
        for h in range(pair * (pw // head_width), (pair + 1) * (pw // head_width)):
            lane0 = (h * head_width) % pw
            done = acc_ref[h] / l_ref[h]
            for g in range(group):
                heads.append(done[g * seq : (g + 1) * seq, lane0 : lane0 + head_width])
        width = len(heads) * head_width
        att_all[t, :, pair * width : (pair + 1) * width] = jnp.concatenate(heads, axis=1).astype(
            jnp.bfloat16
        )

    def a_copy(owner, peer):
        block = att_all.at[owner]
        return rdma(block, block, a_send.at[peer], a_recv.at[owner], "tp", peer)

    def a_relay(owner, part, peer):
        block = att_all.at[owner, pl.ds(part * (seq // 2), seq // 2)]
        return rdma(block, block, af_send.at[part], af_recv.at[part], "tp", peer)

    for peer in peers:
        a_copy(t, peer).start()
    loads[3].wait()
    for owner in peers:
        a_copy(owner, owner).wait_recv()
    if square:
        a_relay(x_peer, 0, y_peer).start()
        a_relay(y_peer, 1, x_peer).start()
        a_relay(far_peer, 0, y_peer).wait_recv()
        a_relay(far_peer, 1, x_peer).wait_recv()
    aw = att_all.shape[2]
    out_cols = attn_ref.shape[1]
    half = math.gcd(out_cols, 256)

    def mix(i, carry):
        at = pl.ds(pl.multiple_of(i * half, half), half)
        total = jnp.zeros((seq, half), jnp.float32)
        for s in range(T):
            total = total + jnp.dot(
                att_all[s], mixer_w[s * aw : (s + 1) * aw, at], preferred_element_type=jnp.float32
            )
        attn_ref[:, at] = total.astype(jnp.bfloat16)
        return carry

    lax.fori_loop(0, out_cols // half, mix, 0)

    def wait_ret(j, carry):
        origin = (e + j) % n
        r_copy(origin, origin).wait_recv()
        return carry

    lax.fori_loop(1, n, wait_ret, 0)
    returned = ret[...].reshape(n * capp, ret.shape[2])
    tokens = moe_ref.shape[0]
    combined = jnp.zeros(moe_ref.shape, jnp.float32)
    for k in range(share_ref.shape[0]):
        combined = combined + share_ref[k] * jnp.dot(
            pick_ref[k], returned, preferred_element_type=jnp.float32
        )
    moe_ref[...] = combined.astype(jnp.bfloat16)

    def drain_ep(j, carry):
        dest = (e + j) % n
        d_copy(dest, e).wait_send()
        r_copy(dest, e).wait_send()
        return carry

    lax.fori_loop(1, n, drain_ep, 0)

    def drain_kv(k, carry):
        zd = chip_to(k)
        kv_copy(zd * CORES + c, None, kv_send.at[zd]).wait_send()
        return carry

    lax.fori_loop(1, nz, drain_kv, 0)

    def drain_tp(k, carry):
        kv_copy(sibling, e, f_send.at[k]).wait_send()
        for p in range(1, T):
            h_copy(k, t, (t + p) % T).wait_send()
        for peer in peers:
            g_copy(k, t, peer).wait_send()
        if square:
            g_relay(k, x_peer, 0, y_peer).wait_send()
            g_relay(k, y_peer, 1, x_peer).wait_send()
        return carry

    lax.fori_loop(0, nz, drain_tp, 0)
    for peer in peers:
        a_copy(t, peer).wait_send()
    if square:
        a_relay(x_peer, 0, y_peer).wait_send()
        a_relay(y_peer, 1, x_peer).wait_send()


def on_device(
    n,
    T,
    query_input,
    key_input,
    value_input,
    query_gain,
    key_gain,
    mixer_out,
    moe_input,
    moe_gain,
    routes,
    route_weight,
    expert_gate,
    expert_up,
    expert_down,
):
    seq_dev = query_input.shape[0]
    head_width = query_gain.shape[0]
    heads_here = query_input.shape[1] // head_width
    kh = key_input.shape[1] // head_width
    kw = key_input.shape[1]
    group = heads_here // kh
    pw = min(128, kw)
    hp = pw // head_width
    positions = lax.axis_index("ep") * seq_dev + jnp.arange(seq_dev, dtype=jnp.int32)
    cosine, sine = rope_tables(positions, head_width)
    query_rot = norm_rotate(query_input, query_gain, cosine, sine, head_width)
    key_rot = norm_rotate(key_input, key_gain, cosine, sine, head_width)
    query_rot = query_rot * jnp.bfloat16(head_width ** (-0.5))
    by_head = []
    for h in range(kh):
        for g in range(group):
            col = (h * group + g) * head_width
            place = (h % hp) * head_width
            by_head.append(
                jnp.pad(
                    query_rot[:, col : col + head_width],
                    ((0, 0), (place, pw - head_width - place)),
                )
            )
    q_pad = jnp.stack(by_head).reshape(kh, group * seq_dev, pw)
    key_value = jnp.stack([key_rot, value_input])

    token_count, model_width = moe_input.shape
    top = routes.shape[1]
    local_experts = expert_gate.shape[0]
    assert local_experts == 1
    expert_count = local_experts * n
    capacity = 3 * token_count * top // (2 * expert_count)
    capp = -(-capacity // 16) * 16
    feat = model_width // T
    flat = routes.reshape(-1)
    pairs = token_count * top
    one_hot = flat[:, None] == jnp.arange(expert_count, dtype=jnp.int32)[None, :]
    order = jnp.arange(pairs, dtype=jnp.int32)
    before = (order[:, None] > order[None, :]).astype(jnp.bfloat16)
    earlier = jnp.dot(before, one_hot.astype(jnp.bfloat16), preferred_element_type=jnp.float32)
    slot = jnp.sum(jnp.where(one_hot, earlier, 0.0), axis=1).astype(jnp.int32)
    places = (flat * capp + slot).reshape(token_count, top)
    slots = jnp.arange(n * capp, dtype=jnp.int32)
    pick = (places.T[:, :, None] == slots[None, None, :]).astype(jnp.bfloat16)
    features = moe_input.astype(jnp.float32)
    inv = lax.rsqrt(jnp.mean(features * features, axis=-1, keepdims=True) + epsilon)
    start = lax.axis_index("tp") * feat
    own = lax.dynamic_slice_in_dim(moe_input, start, feat, 1).astype(jnp.float32)
    normed = (own * inv * lax.dynamic_slice_in_dim(moe_gain, start, feat, 0)).astype(jnp.bfloat16)
    disp = lax.dot_general(
        jnp.sum(pick, axis=0),
        normed,
        (((0,), (0,)), ((), ())),
        preferred_element_type=jnp.float32,
    ).astype(jnp.bfloat16)
    disp = disp.reshape(n, capp, feat)
    shares = route_weight / jnp.sum(route_weight, axis=-1, keepdims=True)
    shares = shares.T[:, :, None]

    gate = expert_gate[0]
    up = expert_up[0]
    down = expert_down[0]
    ffl = gate.shape[1]
    cols = down.shape[1]
    nz = n // CORES
    aw = heads_here * head_width
    out_cols = mixer_out.shape[1]
    bf = jnp.bfloat16
    dma = pltpu.SemaphoreType.DMA
    vmem = pl.BlockSpec(memory_space=pltpu.VMEM)
    hbm = pl.BlockSpec(memory_space=pl.ANY)
    return pl.pallas_call(
        functools.partial(kernel, (n, T, head_width, hp)),
        out_shape=(
            jax.ShapeDtypeStruct((seq_dev, out_cols), bf),
            jax.ShapeDtypeStruct((token_count, cols), bf),
        ),
        in_specs=[vmem] * 5 + [hbm] * 4,
        out_specs=(vmem, vmem),
        scratch_shapes=[
            pltpu.VMEM((n, 2, seq_dev, kw), bf),
            pltpu.VMEM((T, n, capp, feat), bf),
            pltpu.VMEM((T, n, capp, ffl), bf),
            pltpu.VMEM((n, capp, cols), bf),
            pltpu.VMEM((n, capp, cols), bf),
            pltpu.VMEM((T, seq_dev, aw), bf),
            pltpu.VMEM(gate.shape, bf),
            pltpu.VMEM(up.shape, bf),
            pltpu.VMEM(down.shape, bf),
            pltpu.VMEM(mixer_out.shape, bf),
            pltpu.VMEM((kh, group * seq_dev, 1), jnp.float32),
            pltpu.VMEM((kh, group * seq_dev, 1), jnp.float32),
            pltpu.VMEM((kh, group * seq_dev, pw), jnp.float32),
            dma((4,)),
            dma((2,)),
            dma((n,)),
            dma((n,)),
            dma((nz,)),
            dma((n,)),
            dma((nz,)),
            dma((T, nz)),
            dma((T, nz)),
            dma((T, nz)),
            dma((T, nz)),
            dma((n,)),
            dma((n,)),
            dma((T,)),
            dma((T,)),
            dma((2, nz)),
            dma((2, nz)),
            dma((2,)),
            dma((2,)),
        ],
        compiler_params=pltpu.CompilerParams(
            collective_id=0, has_side_effects=True, vmem_limit_bytes=63 * 1024 * 1024
        ),
    )(q_pad, key_value, disp, pick, shares, gate, up, down, mixer_out)


def solution(mesh):
    placed = (
        P("ep", "tp"),
        P("ep", "tp"),
        P("ep", "tp"),
        P(),
        P(),
        P(None, "tp"),
        P("ep", None),
        P(),
        P("ep", None),
        P("ep", None),
        P("ep", None, "tp"),
        P("ep", None, "tp"),
        P("ep", None, "tp"),
    )
    return jax.shard_map(
        functools.partial(on_device, mesh.shape["ep"], mesh.shape["tp"]),
        mesh=mesh,
        in_specs=placed,
        out_specs=(P("ep", "tp"), P("ep", "tp")),
        check_vma=False,
    )
```
